128 devices in a mesh: sp: 64 (over z, y, x), tp: 2 (over core).
Axes of the slice: x: 4, y: 4, z: 4, core: 2. Of those that a mesh axis runs over, the one named last changes fastest.
Arguments:
- residual: bfloat16 [16384, 2048], P(('sp', 'tp')), may hold values from -6 to 6
- projected: bfloat16 [16384, 2048], P('sp', 'tp'), may hold values from -6 to 6
- group_weight: bfloat16 [4, 512, 512], P('tp'), may hold values from -0.25 to 0.25
- channel_scale: float32 [2048], P('tp'), may hold values from 0.1 to 1.9
- out_weight: bfloat16 [2048, 2048], replicated, may hold values from -0.125 to 0.125
- post_mix_gain: float32 [2048], replicated, may hold values from 0.1 to 1.9
- pre_ffn_gain: float32 [2048], replicated, may hold values from 0.1 to 1.9
- post_ffn_gain: float32 [2048], replicated, may hold values from 0.1 to 1.9
- route_ids: int32 [16384, 2], P(('sp', 'tp')), may hold values from 0 to 31, all different within a row; in each aligned block of 128 rows (0 to 127, 128 to 255, ...) at most 16 rows name the same one
- route_weight: float32 [16384, 2], P(('sp', 'tp')), may hold values from 0.1 to 1
- expert_gate: bfloat16 [64, 2048, 1792], P('sp', None, 'tp'), may hold values from -0.125 to 0.125
- expert_up: bfloat16 [64, 2048, 1792], P('sp', None, 'tp'), may hold values from -0.125 to 0.125
- expert_down: bfloat16 [64, 1792, 2048], P('sp', 'tp'), may hold values from -0.09375 to 0.09375
Outputs:
- layer_out: bfloat16 [16384, 2048], P(('sp', 'tp'))
The draws below stay inside these ranges and needn't reach their ends.
Inputs may be any that keep to these rules, and one draw needn't show every extreme that they name: `route_ids`: each row names 2 different experts. In every aligned block of 128 rows (the rows of one device) no expert is named more than 16 times, a bound that some blocks reach.
All inputs are finite; a program needn't handle non-finite values.
Results may differ from the reference program's by a relative error of at most 0.014.
Values may be sent and summed in bfloat16 or wider, within the bound.
A program may use at most 192 MiB of HBM per device.

```python
import math
import jax
import jax.numpy as jnp
import numpy as np
from jax import lax

D = 2048
GROUPS = 4
GROUP_W = 512
FF = 3584
TOP = 2
TOKENS = 16384
ROWS_DEV = 128
EXPERTS = 32
HALVES = 64
CAP = 16
N_SP = 64
N_TP = 2


def steps_of(key, extent, split, low, top_value):
    loudness, own = 1.0, jax.random.fold_in(key, 6)
    for dim, parts in split:
        heights = jnp.exp(jax.random.uniform(jax.random.fold_in(own, dim), (parts,), jnp.float32, low / len(split), top_value / len(split)))
        loudness = loudness * jnp.repeat(heights, extent[dim] // parts).reshape([-1 if axis == dim else 1 for axis in range(len(extent))])
    return loudness


def assign_block(key, own, number, rows, number_of, top, limit, slope):
    sequence = jax.random.permutation(key, number_of)
    heavy_load, usual = load_shares(number_of, rows * top, limit, slope, True), load_shares(number_of, rows * top, limit, slope, False)
    places = jnp.arange(number_of)

    def named(sizes, rotation):
        used = int((sizes > 0).sum())
        fixed = max(1, used // 4)
        passed = fixed + (places - fixed + rotation * (used - fixed)) % max(1, number_of - fixed)
        return jnp.zeros((number_of,), jnp.int32).at[sequence[jnp.where(places < fixed, places, passed)]].set(jnp.asarray(sizes, jnp.int32))

    sizes = jnp.where(number % 4 == 0, named(heavy_load, number // 4), named(usual, number - number // 4 - 1))
    mixed = jax.random.permutation(jax.random.fold_in(own, 3), number_of)
    giver, receiver = mixed[0:number_of // 2 * 2:2], mixed[1:number_of // 2 * 2:2]
    margin = jnp.minimum(sizes[giver] - 1, limit - sizes[receiver]) // 2
    margin = jnp.where((giver == sequence[0]) | (receiver == sequence[0]) | (sizes[receiver] == 0), 0, jnp.maximum(margin, 0))
    passed = jax.random.randint(jax.random.fold_in(own, 4), (number_of // 2,), 0, 1 << 20) % (margin + 1)
    sizes = sizes.at[giver].add(-passed).at[receiver].add(passed)
    members = jnp.searchsorted(jnp.cumsum(sizes), jnp.arange(rows * top), side="right").astype(jnp.int32)
    listing = members.reshape(top, rows).T
    listing = listing[jax.random.permutation(jax.random.fold_in(own, 1), rows)]
    rotation = jax.random.randint(jax.random.fold_in(own, 2), (rows, 1), 0, top)
    return jnp.take_along_axis(listing, (jnp.arange(top)[None, :] + rotation) % top, axis=1)


def load_shares(number_of, total, most, slope, full):
    weights = [(1 << 20) // math.isqrt(grade ** slope) + 1 for grade in range(1, number_of + 1)]
    largest = most if full else min(most, max(-(-total // number_of), total * weights[0] // sum(weights)))
    least = 1 if total - largest >= number_of - 1 else 0
    given, spare = [largest] + [least] * (number_of - 1), total - largest - least * (number_of - 1)
    while spare > 0:
        movable = [i for i in range(1, number_of) if given[i] < largest] or [i for i in range(1, number_of) if given[i] < most]
        pool, remaining = sum([weights[i] for i in movable]), spare
        for i in movable:
            extra = min(most - given[i], max(1, remaining * weights[i] // pool), spare)
            given[i] = given[i] + extra
            spare = spare - extra
    return np.array(given)


def scatter_about(rng, dims, width, limit, shards=(), kind=jnp.bfloat16):
    result = jax.random.normal(rng, dims, jnp.float32) * width
    if len(shards) > 0:
        result = steps_of(rng, dims, shards, -0.22, 0.18) * result
    return jnp.clip(result, min=-limit, max=limit).astype(kind)


def setup_inputs(seed: int = 0) -> dict:
    keys = jax.random.split(jax.random.key(seed), 14)
    residual = scatter_about(keys[0], (TOKENS, D), 1.0, 6.0, ((0, 128),))
    projected = scatter_about(keys[1], (TOKENS, D), 1.0, 6.0, ((0, 64), (1, 2)))
    group_weight = scatter_about(keys[2], (GROUPS, GROUP_W, GROUP_W), GROUP_W ** -0.5, 0.25, ((0, 2),))
    channel_scale = jnp.clip(1.0 + 0.18 * jax.random.normal(keys[3], (D,), jnp.float32), 0.1, 1.9)
    out_weight = scatter_about(keys[4], (D, D), D ** -0.5, 0.125)
    post_mix_gain = jnp.clip(1.0 + 0.18 * jax.random.normal(keys[5], (D,), jnp.float32), 0.1, 1.9)
    pre_ffn_gain = jnp.clip(1.0 + 0.18 * jax.random.normal(keys[6], (D,), jnp.float32), 0.1, 1.9)
    post_ffn_gain = jnp.clip(1.0 + 0.18 * jax.random.normal(keys[7], (D,), jnp.float32), 0.1, 1.9)
    route_ids_keys = jax.random.split(jax.random.fold_in(keys[8], 1), TOKENS // ROWS_DEV)
    route_ids_turns = jax.random.permutation(jax.random.fold_in(keys[8], 3), TOKENS // ROWS_DEV)
    route_ids = jax.vmap(lambda own, number: assign_block(jax.random.fold_in(keys[8], 2), own, number, ROWS_DEV, EXPERTS, TOP, CAP, 2))(route_ids_keys, route_ids_turns).reshape((TOKENS, TOP))
    route_weight = jnp.clip(0.1 + 0.9 * jax.random.uniform(keys[9], (TOKENS, TOP), jnp.float32) ** steps_of(keys[9], (TOKENS, TOP), ((0, 128),), -0.2, 0.2), 0.1, 1.0)
    expert_gate = scatter_about(keys[10], (HALVES, D, FF // 2), D ** -0.5, 0.125, ((0, 64), (2, 2)))
    expert_up = scatter_about(keys[11], (HALVES, D, FF // 2), D ** -0.5, 0.125, ((0, 64), (2, 2)))
    expert_down = scatter_about(keys[12], (HALVES, FF // 2, D), FF ** -0.5, 0.09375, ((0, 64), (1, 2)))
    return dict(residual=residual, projected=projected, group_weight=group_weight, channel_scale=channel_scale, out_weight=out_weight, post_mix_gain=post_mix_gain, pre_ffn_gain=pre_ffn_gain, post_ffn_gain=post_ffn_gain, route_ids=route_ids, route_weight=route_weight, expert_gate=expert_gate, expert_up=expert_up, expert_down=expert_down)


EPS = 1e-06

def rms_scale(values, gain):
    values = values.astype(jnp.float32)
    inverse = lax.rsqrt(lax.optimization_barrier(jnp.mean(values * values, axis=-1, keepdims=True)) + EPS)
    return values * inverse * gain.astype(jnp.float32)

def window_sums(extended, lookback, count):
    levels = []
    current = extended
    window_span = 1
    for level_id in range(GROUPS):
        current = current[window_span:] + current[:-window_span]
        window_span = window_span * 2
        first = lookback - window_span + 1
        levels.append(lax.slice_in_dim(current, first, first + count, axis=0))
    return levels

def expert_output(token_rows, expert_id, expert_gate, expert_up, expert_down):
    quarter = FF // (2 * N_TP)
    total = jnp.zeros((token_rows.shape[0], D), jnp.float32)
    for half_id in range(2):
        entry = (2 * expert_id + half_id).astype(jnp.int32)
        gate_half = lax.dynamic_index_in_dim(expert_gate, entry, 0, keepdims=False)
        up_half = lax.dynamic_index_in_dim(expert_up, entry, 0, keepdims=False)
        down_half = lax.dynamic_index_in_dim(expert_down, entry, 0, keepdims=False)
        partial_value = jnp.zeros((token_rows.shape[0], D), jnp.float32)
        for part_id in range(N_TP):
            low = part_id * quarter
            gate_value = jnp.dot(token_rows, gate_half[:, low:low + quarter], preferred_element_type=jnp.float32)
            up_value = jnp.dot(token_rows, up_half[:, low:low + quarter], preferred_element_type=jnp.float32)
            active = (jax.nn.silu(gate_value) * up_value).astype(jnp.bfloat16)
            term = jnp.dot(active, down_half[low:low + quarter], preferred_element_type=jnp.float32).astype(jnp.bfloat16)
            partial_value = partial_value + term.astype(jnp.float32)
        total = total + partial_value.astype(jnp.bfloat16).astype(jnp.float32)
    rounded = lax.optimization_barrier(total.astype(jnp.bfloat16))
    return rounded.astype(jnp.float32)

def reference(residual, projected, group_weight, channel_scale, out_weight, post_mix_gain, pre_ffn_gain, post_ffn_gain, route_ids, route_weight, expert_gate, expert_up, expert_down):
    lookback = 2 ** GROUPS
    count = projected.shape[0]
    extended = jnp.concatenate([jnp.zeros((lookback, D), jnp.float32), projected.astype(jnp.float32)], 0)
    levels = window_sums(extended, lookback, count)
    position = (jnp.arange(count, dtype=jnp.int32) + 1).astype(jnp.float32)[:, None]
    pieces = []
    for group_id in range(GROUPS):
        low = group_id * GROUP_W
        window_span = jnp.float32(2.0 ** (group_id + 1))
        own_part = projected[:, low:low + GROUP_W].astype(jnp.float32)
        pieces.append(levels[group_id][:, low:low + GROUP_W] / jnp.minimum(position, window_span) - own_part)
    pooled = jnp.concatenate(pieces, 1).astype(jnp.bfloat16)
    grouped = jnp.einsum('tgc,gce->tge', pooled.reshape(count, GROUPS, GROUP_W).astype(jnp.float32), group_weight.astype(jnp.float32))
    scaled = (grouped.reshape(count, D) * channel_scale.astype(jnp.float32)).astype(jnp.bfloat16)
    mixed = jnp.dot(scaled, out_weight, preferred_element_type=jnp.float32).astype(jnp.bfloat16)
    middle = (residual.astype(jnp.float32) + rms_scale(mixed, post_mix_gain)).astype(jnp.bfloat16)
    normed = rms_scale(middle, pre_ffn_gain).astype(jnp.bfloat16)
    flat_ids = route_ids.reshape(-1).astype(jnp.int32)
    flat_weight = route_weight.reshape(-1).astype(jnp.float32)
    order = jnp.argsort(flat_ids, stable=True).astype(jnp.int32)
    onehot = (flat_ids[:, None] == jnp.arange(EXPERTS, dtype=jnp.int32)[None, :]).astype(jnp.int32)
    counts = lax.optimization_barrier(jnp.sum(onehot, 0)).astype(jnp.int32)
    starts = (jnp.cumsum(counts) - counts).astype(jnp.int32)
    most = CAP * N_SP * N_TP
    order_padded = jnp.concatenate([order, jnp.zeros((most,), jnp.int32)])

    def add_expert(total, expert_id):
        picks = lax.dynamic_slice_in_dim(order_padded, starts[expert_id].astype(jnp.int32), most)
        live = jnp.arange(most, dtype=jnp.int32) < counts[expert_id]
        token_ids = (picks // TOP).astype(jnp.int32)
        outputs = expert_output(normed[token_ids], expert_id, expert_gate, expert_up, expert_down)
        factor = jnp.where(live, flat_weight[picks], jnp.float32(0.0))
        return (total.at[token_ids].add(outputs * factor[:, None]), None)
    ffn_sum, _ = lax.scan(add_expert, jnp.zeros((count, D), jnp.float32), jnp.arange(EXPERTS, dtype=jnp.int32))
    return (middle.astype(jnp.float32) + rms_scale(ffn_sum, post_ffn_gain)).astype(jnp.bfloat16)
```

```python
import functools

import jax
import jax.numpy as jnp
from jax import lax
from jax.experimental import pallas as pl
from jax.experimental.pallas import tpu as pltpu
from jax.sharding import PartitionSpec as P

EPS = 1e-06
MESH = pl.DeviceIdType.MESH
F32 = jnp.float32
BF16 = jnp.bfloat16
SIDE = 4
WAVES = 4
TILE = 256


def dot(a, b):
    return jnp.dot(a, b, preferred_element_type=F32)


def flag(condition):
    return jnp.where(condition, 1.0, 0.0).astype(F32)


def layer(
    res_h, proj_h, gw_h, cs, ow_h, post_mix, pre_ffn, post_ffn, ids_t, ids, wts, eg_h, eu_h, ed_h,
    out,
    pbuf, gw, ow, res, scaled, token, mid, normed, pick, table, rbuf, obuf, rr, gf, uf, df, act, wcat,
    proj_acc, lsem, wsem, wrem, hsem, tsem, dsend, drecv, rsend, rrecv,
):
    sp = lax.axis_index("sp")
    tp = lax.axis_index("tp")
    other = 1 - tp
    n_sp = lax.axis_size("sp")
    z, y, x = sp // (SIDE * SIDE), (sp // SIDE) % SIDE, sp % SIDE
    rows = out.shape[0]
    width = out.shape[1]
    half_width = width // 2
    cap = table.shape[0] // (n_sp // 2)
    quarter = eg_h.shape[2]
    look = pbuf.shape[0] - 2 * rows
    per_wave = n_sp // WAVES

    def offsets(k):
        c, i = k // per_wave, k % per_wave
        dx, dy = i % SIDE, i // SIDE
        return (c + 2 * SIDE - dx - dy) % SIDE, dy, dx

    def ahead(k):
        dz, dy, dx = offsets(k)
        return ((z + dz) % SIDE) * SIDE * SIDE + ((y + dy) % SIDE) * SIDE + (x + dx) % SIDE

    def behind(k):
        dz, dy, dx = offsets(k)
        return (
            ((z + SIDE - dz) % SIDE) * SIDE * SIDE
            + ((y + SIDE - dy) % SIDE) * SIDE
            + (x + SIDE - dx) % SIDE
        )

    barrier = pltpu.get_barrier_semaphore()

    def greet(k, carry):
        pl.semaphore_signal(barrier, inc=1, device_id=(ahead(k), tp), device_id_type=MESH)
        return carry

    lax.fori_loop(1, n_sp, greet, 0)
    pl.semaphore_signal(barrier, inc=1, device_id=(sp, other), device_id_type=MESH)

    own_cols = pl.ds(pl.multiple_of(tp * quarter, 128), quarter)
    own_rows = pl.ds(pl.multiple_of(tp * quarter, 128), quarter)
    local = [
        pltpu.make_async_copy(proj_h, pbuf.at[pl.ds(look, 2 * rows)], lsem.at[0]),
        pltpu.make_async_copy(gw_h, gw, lsem.at[1]),
        pltpu.make_async_copy(ow_h, ow, lsem.at[2]),
        pltpu.make_async_copy(res_h, res, lsem.at[3]),
        pltpu.make_async_copy(eg_h.at[0], gf.at[:, own_cols], lsem.at[4]),
        pltpu.make_async_copy(eu_h.at[0], uf.at[:, own_cols], lsem.at[5]),
        pltpu.make_async_copy(ed_h.at[0], df.at[own_rows], lsem.at[6]),
    ]
    for copy in local:
        copy.start()

    experts = n_sp // 2
    e_sub = lax.broadcasted_iota(jnp.int32, (experts, rows), 0)
    named_t = flag(e_sub == ids_t[0:1, :]) + flag(e_sub == ids_t[1:2, :])
    r0 = lax.broadcasted_iota(jnp.int32, (rows, rows), 0)
    r1 = lax.broadcasted_iota(jnp.int32, (rows, rows), 1)
    before_t = dot(named_t.astype(BF16), flag(r0 < r1).astype(BF16))
    slots = experts * cap
    s0 = lax.broadcasted_iota(jnp.int32, (slots, experts), 0)
    s1 = lax.broadcasted_iota(jnp.int32, (slots, experts), 1)
    spread_t = flag(s0 // cap == s1).astype(BF16)
    named_slot = dot(spread_t, named_t.astype(BF16))
    before_slot = dot(spread_t, before_t.astype(BF16))
    place = (lax.broadcasted_iota(jnp.int32, (slots, rows), 0) % cap).astype(F32)
    pick[...] = flag((named_slot > 0.5) & (before_slot == place)).astype(BF16)

    e_lane = lax.broadcasted_iota(jnp.int32, (rows, experts), 1)
    first, second = flag(e_lane == ids[:, 0:1]), flag(e_lane == ids[:, 1:2])
    named = first + second
    before = dot(flag(r1 < r0).astype(BF16), named.astype(BF16))
    weight = first * wts[:, 0:1] + second * wts[:, 1:2]
    high = weight.astype(BF16)
    low = (weight - high.astype(F32)).astype(BF16)
    q0 = lax.broadcasted_iota(jnp.int32, (experts, 2 * slots), 0)
    q1 = lax.broadcasted_iota(jnp.int32, (experts, 2 * slots), 1)
    spread = flag(q1 // (2 * cap) == q0).astype(BF16)
    lane_place = (lax.broadcasted_iota(jnp.int32, (rows, 2 * slots), 1) % cap).astype(F32)
    here = (dot(named.astype(BF16), spread) > 0.5) & (dot(before.astype(BF16), spread) == lane_place)
    wcat[0:rows] = jnp.where(here, dot(high, spread), 0.0).astype(BF16)
    wcat[rows : 2 * rows] = jnp.where(here, dot(low, spread), 0.0).astype(BF16)

    local[0].wait()
    pl.semaphore_wait(barrier, n_sp)

    halo = pltpu.make_async_remote_copy(
        src_ref=pbuf.at[pl.ds(2 * rows, look)],
        dst_ref=pbuf.at[pl.ds(0, look)],
        send_sem=hsem.at[0],
        recv_sem=hsem.at[1],
        device_id=((sp + 1) % n_sp, tp),
        device_id_type=MESH,
    )
    halo.start()
    pushes = [
        pltpu.make_async_remote_copy(
            src_ref=src, dst_ref=dst, send_sem=wsem.at[i], recv_sem=wrem.at[i],
            device_id=(sp, other), device_id_type=MESH,
        )
        for i, (src, dst) in enumerate(
            (
                (eg_h.at[0], gf.at[:, own_cols]),
                (eu_h.at[0], uf.at[:, own_cols]),
                (ed_h.at[0], df.at[own_rows]),
            )
        )
    ]
    for push in pushes:
        push.start()

    halo.wait()
    local[1].wait()
    group = gw.shape[1]
    total = pbuf.shape[0]
    row_id = lax.broadcasted_iota(jnp.int32, (total, group), 0)
    position = (row_id - look + 1 + sp * (2 * rows)).astype(F32)
    for lg in range(2):
        cols = slice(lg * group, (lg + 1) * group)
        own = pbuf[:, cols].astype(F32)
        own = jnp.where((row_id >= look) | (sp > 0), own, 0.0)
        sums = [own]
        for level in range(4):
            sums.append(pltpu.roll(sums[-1], 2**level, 0) + sums[-1])
        summed = jnp.where(tp == 0, sums[lg + 1], sums[lg + 3])
        span = jnp.where(tp == 0, F32(2.0 ** (lg + 1)), F32(2.0 ** (lg + 3)))
        pooled = (summed / jnp.minimum(position, span) - own).astype(BF16)[look:]
        scaled[:, cols] = (dot(pooled, gw[lg]) * cs[:, cols]).astype(BF16)

    swap = pltpu.make_async_remote_copy(
        src_ref=scaled.at[pl.ds(pl.multiple_of(other * rows, rows), rows)],
        dst_ref=token,
        send_sem=tsem.at[0],
        recv_sem=tsem.at[1],
        device_id=(sp, other),
        device_id_type=MESH,
    )
    swap.start()
    local[2].wait()
    local[3].wait()
    mine = pl.ds(pl.multiple_of(tp * rows, rows), rows)

    def project(source, part, accumulate):
        def step(n, carry):
            cols = pl.ds(pl.multiple_of(n * TILE, TILE), TILE)
            block = ow[pl.ds(pl.multiple_of(part * half_width, half_width), half_width), cols]
            value = dot(source, block)
            proj_acc[:, cols] = proj_acc[:, cols] + value if accumulate else value
            return carry

        lax.fori_loop(0, width // TILE, step, 0)

    project(scaled[mine], tp, False)
    swap.wait()
    project(token[...], other, True)

    mixed = proj_acc[...].astype(BF16).astype(F32)
    inverse = lax.rsqrt(jnp.mean(mixed * mixed, axis=-1, keepdims=True) + EPS)
    middle = (res[...].astype(F32) + mixed * inverse * post_mix[...]).astype(BF16)
    mid[...] = middle
    middle = middle.astype(F32)
    inverse = lax.rsqrt(jnp.mean(middle * middle, axis=-1, keepdims=True) + EPS)
    normed[...] = (middle * inverse * pre_ffn[...]).astype(BF16)

    def fill(n, carry):
        block = pl.ds(pl.multiple_of(n * rows, rows), rows)
        table[block] = dot(pick[block], normed[...]).astype(BF16)
        return carry

    lax.fori_loop(0, slots // rows, fill, 0)

    def outgoing(k):
        peer = ahead(k)
        return pltpu.make_async_remote_copy(
            src_ref=table.at[pl.ds(pl.multiple_of((peer // 2) * cap, cap), cap)],
            dst_ref=rbuf.at[k // per_wave, pl.ds(pl.multiple_of((k % per_wave) * cap, cap), cap)],
            send_sem=dsend.at[k],
            recv_sem=drecv.at[k],
            device_id=(peer, tp),
            device_id_type=MESH,
        )

    def returning(k):
        return pltpu.make_async_remote_copy(
            src_ref=obuf.at[k // per_wave, pl.ds(pl.multiple_of((k % per_wave) * cap, cap), cap)],
            dst_ref=rr.at[pl.ds(pl.multiple_of(sp * cap, cap), cap)],
            send_sem=rsend.at[k],
            recv_sem=rrecv.at[k],
            device_id=(behind(k), tp),
            device_id_type=MESH,
        )

    def each(low, high, act_on):
        def step(k, carry):
            act_on(k)
            return carry

        lax.fori_loop(low, high, step, 0)

    each(1, n_sp, lambda k: outgoing(k).start())
    rbuf[0, 0:cap] = table[pl.ds(pl.multiple_of((sp // 2) * cap, cap), cap)]

    for copy in local[4:]:
        copy.wait()
    for push in pushes:
        push.wait()

    hidden = gf.shape[1]
    for c in range(WAVES):
        low = 1 if c == 0 else c * per_wave
        each(low, (c + 1) * per_wave, lambda k: outgoing(k).wait_recv())

        def hid(n, carry):
            cols = pl.ds(pl.multiple_of(n * TILE, TILE), TILE)
            gate = dot(rbuf[c], gf[:, cols])
            up = dot(rbuf[c], uf[:, cols])
            act[:, cols] = (jax.nn.silu(gate) * up).astype(BF16)
            return carry

        lax.fori_loop(0, hidden // TILE, hid, 0)

        def down(n, carry):
            cols = pl.ds(pl.multiple_of(n * TILE, TILE), TILE)
            obuf[c, :, cols] = dot(act[...], df[:, cols]).astype(BF16)
            return carry

        lax.fori_loop(0, width // TILE, down, 0)
        each(low, (c + 1) * per_wave, lambda k: returning(k).start())
    rr[pl.ds(pl.multiple_of(sp * cap, cap), cap)] = obuf[0, 0:cap]

    each(1, n_sp, lambda k: outgoing(k).wait_send())
    each(1, n_sp, lambda k: returning(k).wait_recv())

    def combine(n, carry):
        cols = pl.ds(pl.multiple_of(n * TILE, TILE), TILE)
        both = dot(wcat[...], rr[:, cols])
        proj_acc[:, cols] = both[0:rows] + both[rows : 2 * rows]
        return carry

    lax.fori_loop(0, width // TILE, combine, 0)
    ffn = proj_acc[...]
    inverse = lax.rsqrt(jnp.mean(ffn * ffn, axis=-1, keepdims=True) + EPS)
    out[...] = (mid[...].astype(F32) + ffn * inverse * post_ffn[...]).astype(BF16)
    each(1, n_sp, lambda k: returning(k).wait_send())


def body(
    residual, projected, group_weight, channel_scale, out_weight, post_mix_gain, pre_ffn_gain,
    post_ffn_gain, route_ids, route_weight, expert_gate, expert_up, expert_down,
):
    n_sp = lax.axis_size("sp")
    rows, width = residual.shape
    lines, local_width = projected.shape
    look = 16
    slots = n_sp // 2 * (4 * rows // (n_sp // 2))
    cap = slots // (n_sp // 2)
    quarter = expert_gate.shape[2]
    hidden = 2 * quarter
    wave_rows = n_sp // WAVES * cap
    any_, vmem = pl.BlockSpec(memory_space=pl.ANY), pl.BlockSpec(memory_space=pltpu.VMEM)
    dma = pltpu.SemaphoreType.DMA
    return pl.pallas_call(
        layer,
        name="layer",
        out_shape=jax.ShapeDtypeStruct((rows, width), BF16),
        in_specs=[any_, any_, any_, vmem, any_, vmem, vmem, vmem, vmem, vmem, vmem, any_, any_, any_],
        out_specs=vmem,
        scratch_shapes=[
            pltpu.VMEM((look + lines, local_width), BF16),
            pltpu.VMEM(group_weight.shape, BF16),
            pltpu.VMEM(out_weight.shape, BF16),
            pltpu.VMEM((rows, width), BF16),
            pltpu.VMEM((lines, local_width), BF16),
            pltpu.VMEM((rows, local_width), BF16),
            pltpu.VMEM((rows, width), BF16),
            pltpu.VMEM((rows, width), BF16),
            pltpu.VMEM((slots, rows), BF16),
            pltpu.VMEM((slots, width), BF16),
            pltpu.VMEM((WAVES, wave_rows, width), BF16),
            pltpu.VMEM((WAVES, wave_rows, width), BF16),
            pltpu.VMEM((2 * slots, width), BF16),
            pltpu.VMEM((width, hidden), BF16),
            pltpu.VMEM((width, hidden), BF16),
            pltpu.VMEM((hidden, width), BF16),
            pltpu.VMEM((wave_rows, hidden), BF16),
            pltpu.VMEM((2 * rows, 2 * slots), BF16),
            pltpu.VMEM((rows, width), F32),
            dma((7,)),
            dma((3,)),
            dma((3,)),
            dma((2,)),
            dma((2,)),
            dma((n_sp,)),
            dma((n_sp,)),
            dma((n_sp,)),
            dma((n_sp,)),
        ],
        compiler_params=pltpu.CompilerParams(
            collective_id=0, has_side_effects=True, vmem_limit_bytes=66_000_000
        ),
    )(
        residual, projected, group_weight, channel_scale.reshape(1, -1), out_weight,
        post_mix_gain.reshape(1, -1), pre_ffn_gain.reshape(1, -1), post_ffn_gain.reshape(1, -1),
        route_ids.T, route_ids, route_weight, expert_gate, expert_up, expert_down,
    )


def solution(mesh):
    in_specs = (
        P(("sp", "tp"), None),
        P("sp", "tp"),
        P("tp", None, None),
        P("tp"),
        P(),
        P(),
        P(),
        P(),
        P(("sp", "tp"), None),
        P(("sp", "tp"), None),
        P("sp", None, "tp"),
        P("sp", None, "tp"),
        P("sp", "tp", None),
    )
    out_specs = P(("sp", "tp"), None)
    return jax.shard_map(body, mesh=mesh, in_specs=in_specs, out_specs=out_specs, check_vma=False)
```

```python
import functools

import jax
import jax.numpy as jnp
from jax import lax
from jax.experimental import pallas as pl
from jax.experimental.pallas import tpu as pltpu
from jax.sharding import PartitionSpec as P

EPS = 1e-06
MESH = pl.DeviceIdType.MESH
F32 = jnp.float32
BF16 = jnp.bfloat16
SIDE = 4
PART = 8
TILE = 256


def dot(a, b):
    return jnp.dot(a, b, preferred_element_type=F32)


def flag(condition):
    return jnp.where(condition, 1.0, 0.0).astype(F32)


def layer(
    res_h, proj_h, gw_h, cs, ow_h, post_mix, pre_ffn, post_ffn, ids_t, wts_t, eg_h, eu_h, ed_h,
    out,
    pbuf, gw, ow, res, scaled, token, mid, normed, raw, pick, table, rbuf, obuf, hbuf, rr, gf, uf, df,
    act, wown, wcross, wpair, acc, pout, pin, ids_t2, wts_t2,
    lsem, wsem, wrem, hsem, tsem, xsend, xrecv, bsend, brecv,
):
    sp = lax.axis_index("sp")
    tp = lax.axis_index("tp")
    other = 1 - tp
    n_sp = lax.axis_size("sp")
    z, y, x = sp // (SIDE * SIDE), (sp // SIDE) % SIDE, sp % SIDE
    rows = out.shape[0]
    width = out.shape[1]
    half_width = width // 2
    cap = 4 * rows // (n_sp // 2)
    quarter = eg_h.shape[2]
    look = pbuf.shape[0] - 2 * rows
    columns = SIDE * SIDE
    slots = columns * cap
    zy = z * SIDE + y
    pair = x // 2
    facing = SIDE - 1 - x
    twin = sp + 1 - 2 * (x % 2)

    def step_of(j):
        dy = j % SIDE
        return (j // SIDE + SIDE - dy) % SIDE, dy

    def ahead(j):
        dz, dy = step_of(j)
        return ((z + dz) % SIDE) * SIDE + (y + dy) % SIDE

    def behind(j):
        dz, dy = step_of(j)
        return ((z + SIDE - dz) % SIDE) * SIDE + (y + SIDE - dy) % SIDE

    def block(j):
        return pl.ds(pl.multiple_of(j * cap, cap), cap)

    def spot(kind, j):
        if kind < 2:
            return kind, block(j)
        return 2 + j // PART, block(j % PART + PART * (kind - 2))

    def each(low, high, act_on):
        def step(k, carry):
            act_on(k)
            return carry

        lax.fori_loop(low, high, step, 0)

    def remote(src, dst, send, recv, device):
        return pltpu.make_async_remote_copy(
            src_ref=src, dst_ref=dst, send_sem=send, recv_sem=recv, device_id=device, device_id_type=MESH
        )

    barrier = pltpu.get_barrier_semaphore()

    def greet(device):
        pl.semaphore_signal(barrier, inc=1, device_id=device, device_id_type=MESH)

    each(1, columns, lambda j: greet((ahead(j) * SIDE + x, tp)))
    each(0, columns, lambda j: greet((ahead(j) * SIDE + facing, tp)))
    greet((twin, tp))
    greet((sp, other))

    own_cols = pl.ds(pl.multiple_of(tp * quarter, 128), quarter)
    own_rows = pl.ds(pl.multiple_of(tp * quarter, 128), quarter)
    local = [
        pltpu.make_async_copy(proj_h, pbuf.at[pl.ds(look, 2 * rows)], lsem.at[0]),
        pltpu.make_async_copy(gw_h, gw, lsem.at[1]),
        pltpu.make_async_copy(ow_h, ow, lsem.at[2]),
        pltpu.make_async_copy(res_h, res, lsem.at[3]),
        pltpu.make_async_copy(eg_h.at[0], gf.at[:, own_cols], lsem.at[4]),
        pltpu.make_async_copy(eu_h.at[0], uf.at[:, own_cols], lsem.at[5]),
        pltpu.make_async_copy(ed_h.at[0], df.at[own_rows], lsem.at[6]),
    ]
    for copy in local:
        copy.start()

    experts = n_sp // 2
    r0 = lax.broadcasted_iota(jnp.int32, (rows, rows), 0)
    r1 = lax.broadcasted_iota(jnp.int32, (rows, rows), 1)
    e_sub = lax.broadcasted_iota(jnp.int32, (experts, rows), 0)
    e_lane = lax.broadcasted_iota(jnp.int32, (rows, experts), 1)
    s0 = lax.broadcasted_iota(jnp.int32, (slots, experts), 0)
    s1 = lax.broadcasted_iota(jnp.int32, (slots, experts), 1)
    q0 = lax.broadcasted_iota(jnp.int32, (experts, slots), 0)
    q1 = lax.broadcasted_iota(jnp.int32, (experts, slots), 1)
    place = (lax.broadcasted_iota(jnp.int32, (slots, rows), 0) % cap).astype(F32)
    lane_place = (lax.broadcasted_iota(jnp.int32, (rows, slots), 1) % cap).astype(F32)

    def named_slots(names):
        named = flag(e_sub == names[0:1, :]) + flag(e_sub == names[1:2, :])
        return named.astype(BF16), dot(named.astype(BF16), flag(r0 < r1).astype(BF16)).astype(BF16)

    def picks(slot_info, side):
        spread = flag((s0 // cap) * 2 + side == s1).astype(BF16)
        hit = dot(spread, slot_info[0]) > 0.5
        return flag(hit & (dot(spread, slot_info[1]) == place)).astype(BF16)

    def row_info(names, values):
        sheet = [names[0:2, :].astype(F32), values[0:2, :], jnp.zeros((4, rows), F32)]
        sheet = jnp.transpose(jnp.concatenate(sheet, axis=0))
        lane = e_lane.astype(F32)
        first, second = flag(lane == sheet[:, 0:1]), flag(lane == sheet[:, 1:2])
        named = (first + second).astype(BF16)
        before = dot(flag(r1 < r0).astype(BF16), named).astype(BF16)
        weight = first * sheet[:, 2:3] + second * sheet[:, 3:4]
        high = weight.astype(BF16)
        return named, before, high, (weight - high.astype(F32)).astype(BF16)

    def weigh(ref, info, side):
        named, before, high, low = info
        spread = flag((q1 // cap) * 2 + side == q0).astype(BF16)
        here = (dot(named, spread) > 0.5) & (dot(before, spread) == lane_place)
        ref[0:rows] = jnp.where(here, dot(high, spread), 0.0).astype(BF16)
        ref[rows : 2 * rows] = jnp.where(here, dot(low, spread), 0.0).astype(BF16)

    own_slots = named_slots(ids_t)
    pick[0] = picks(own_slots, pair)
    pick[1] = picks(own_slots, 1 - pair)
    own_info = row_info(ids_t, wts_t)
    weigh(wown, own_info, pair)
    weigh(wcross, own_info, 1 - pair)

    local[0].wait()
    pl.semaphore_wait(barrier, 2 * columns + 1)
    notes = [
        remote(src, dst, bsend.at[i], brecv.at[i], (twin, tp))
        for i, (src, dst) in enumerate(((ids_t, ids_t2), (wts_t, wts_t2)))
    ]

    halo = remote(
        pbuf.at[pl.ds(2 * rows, look)], pbuf.at[pl.ds(0, look)], hsem.at[0], hsem.at[1],
        ((sp + 1) % n_sp, tp),
    )
    halo.start()
    for note in notes:
        note.start()
    pushes = [
        remote(src, dst, wsem.at[i], wrem.at[i], (sp, other))
        for i, (src, dst) in enumerate(
            (
                (eg_h.at[0], gf.at[:, own_cols]),
                (eu_h.at[0], uf.at[:, own_cols]),
                (ed_h.at[0], df.at[own_rows]),
            )
        )
    ]

    local[1].wait()
    group = gw.shape[1]

    def pool(extended, lg, start, known):
        count = extended.shape[0]
        row_id = lax.broadcasted_iota(jnp.int32, (count, group), 0)
        own = extended.astype(F32)
        if known is not None:
            own = jnp.where((row_id >= look) | known, own, 0.0)
        sums = [own]
        for level in range(4):
            sums.append(pltpu.roll(sums[-1], 2**level, 0) + sums[-1])
        summed = jnp.where(tp == 0, sums[lg + 1], sums[lg + 3])
        span = jnp.where(tp == 0, F32(2.0 ** (lg + 1)), F32(2.0 ** (lg + 3)))
        position = (row_id - look + 1 + start + sp * (2 * rows)).astype(F32)
        return (summed / jnp.minimum(position, span) - own).astype(BF16)[look:]

    def columns_of(lg):
        return slice(lg * group, (lg + 1) * group)

    for lg in range(2):
        cols = columns_of(lg)
        pooled = pool(pbuf[look:, cols], lg, look, None)
        scaled[look:, cols] = (dot(pooled, gw[lg]) * cs[:, cols]).astype(BF16)
    halo.wait()
    for lg in range(2):
        cols = columns_of(lg)
        pooled = pool(pbuf[0 : 2 * look, cols], lg, 0, sp > 0)
        scaled[0:look, cols] = (dot(pooled, gw[lg]) * cs[:, cols]).astype(BF16)

    swap = remote(
        scaled.at[pl.ds(pl.multiple_of(other * rows, rows), rows)], token, tsem.at[0], tsem.at[1],
        (sp, other),
    )
    swap.start()
    local[2].wait()
    local[3].wait()
    mine = pl.ds(pl.multiple_of(tp * rows, rows), rows)

    def project(source, part, accumulate):
        def step(n, carry):
            cols = pl.ds(pl.multiple_of(n * TILE, TILE), TILE)
            part_rows = ow[pl.ds(pl.multiple_of(part * half_width, half_width), half_width), cols]
            value = dot(source, part_rows)
            acc[:, cols] = acc[:, cols] + value if accumulate else value
            return carry

        lax.fori_loop(0, width // TILE, step, 0)

    project(scaled[mine], tp, False)
    swap.wait()
    for push in pushes:
        push.start()
    project(token[...], other, True)

    mixed = acc[...].astype(BF16).astype(F32)
    inverse = lax.rsqrt(jnp.mean(mixed * mixed, axis=-1, keepdims=True) + EPS)
    middle = (res[...].astype(F32) + mixed * inverse * post_mix[...]).astype(BF16)
    mid[...] = middle
    middle = middle.astype(F32)
    inverse = lax.rsqrt(jnp.mean(middle * middle, axis=-1, keepdims=True) + EPS)
    normed[...] = (middle * inverse * pre_ffn[...]).astype(BF16)

    raw_copy = remote(normed, raw, bsend.at[3], brecv.at[3], (twin, tp))
    raw_copy.start()

    def fill(kind, source):
        def step(n, carry):
            cols = pl.ds(pl.multiple_of(n * TILE, TILE), TILE)
            table[kind, :, cols] = dot(pick[kind], source[:, cols]).astype(BF16)
            return carry

        lax.fori_loop(0, width // TILE, step, 0)

    def outgoing(kind, j):
        peer = ahead(j)
        line = facing if kind == 2 else x
        return remote(
            table.at[(0, 2, 1)[kind], block(peer)], rbuf.at[spot(kind, j)],
            xsend.at[kind, j], xrecv.at[kind, j], (peer * SIDE + line, tp),
        )

    def pass_on(j):
        return remote(rbuf.at[spot(2, j)], rbuf.at[spot(3, j)], xsend.at[3, j], xrecv.at[3, j], (twin, tp))

    def returning(kind, j):
        line = facing if kind == 2 else x
        return remote(
            obuf.at[spot(kind, j)], rr.at[kind, block(zy)],
            xsend.at[4 + kind, j], xrecv.at[4 + kind, j], (behind(j) * SIDE + line, tp),
        )

    def halves(j):
        return remote(obuf.at[spot(3, j)], hbuf.at[block(j)], xsend.at[7, j], xrecv.at[7, j], (twin, tp))

    fill(1, normed)
    each(0, columns, lambda j: outgoing(2, j).start())
    fill(0, normed)
    each(1, columns, lambda j: outgoing(0, j).start())
    rbuf[0, 0:cap] = table[0, block(zy)]

    def relay(j):
        outgoing(2, j).wait_recv()
        pass_on(j).start()

    for note in notes:
        note.wait()
    pick[2] = picks(named_slots(ids_t2), pair)
    weigh(wpair, row_info(ids_t2, wts_t2), pair)
    each(0, PART, relay)
    raw_copy.wait_recv()
    fill(2, raw)
    each(1, columns, lambda j: outgoing(1, j).start())
    rbuf[1, 0:cap] = table[2, block(zy)]

    for copy in local[4:]:
        copy.wait()
    for push in pushes:
        push.wait()

    hidden = gf.shape[1]

    def experts_on(c, hook):
        def hid(n, carry):
            cols = pl.ds(pl.multiple_of(n * TILE, TILE), TILE)
            gate = dot(rbuf[c], gf[:, cols])
            up = dot(rbuf[c], uf[:, cols])
            act[:, cols] = (jax.nn.silu(gate) * up).astype(BF16)
            return carry

        lax.fori_loop(0, hidden // TILE, hid, 0)

        def down(n, carry):
            cols = pl.ds(pl.multiple_of(n * TILE, TILE), TILE)
            hook(n)
            obuf[c, :, cols] = dot(act[...], df[:, cols]).astype(BF16)
            return carry

        lax.fori_loop(0, width // TILE, down, 0)

    def nothing(n):
        pass

    each(1, columns, lambda j: outgoing(0, j).wait_recv())
    experts_on(0, lambda n: relay(PART + n))
    each(1, columns, lambda j: returning(0, j).start())
    rr[0, block(zy)] = obuf[0, 0:cap]

    def join(j):
        halves(j).wait_recv()
        both = obuf[spot(2, j)].astype(F32) + hbuf[block(j)].astype(F32)
        obuf[spot(2, j)] = both.astype(BF16)
        returning(2, j).start()

    each(0, PART, lambda j: pass_on(j).wait_recv())
    experts_on(2, nothing)
    each(0, PART, lambda j: halves(j).start())

    each(1, columns, lambda j: outgoing(1, j).wait_recv())
    experts_on(1, nothing)
    each(1, columns, lambda j: returning(1, j).start())
    rr[1, block(zy)] = obuf[1, 0:cap]

    each(PART, columns, lambda j: pass_on(j).wait_recv())
    experts_on(3, join)
    each(PART, columns, lambda j: halves(j).start())

    def combine(weights, kind, cols):
        both = dot(weights[...], rr[kind, :, cols])
        return both[0:rows] + both[rows : 2 * rows]

    each(1, columns, lambda j: returning(1, j).wait_recv())

    def give(n, carry):
        cols = pl.ds(pl.multiple_of(n * TILE, TILE), TILE)
        pout[:, cols] = combine(wpair, 1, cols).astype(BF16)
        return carry

    lax.fori_loop(0, width // TILE, give, 0)
    part_copy = remote(pout, pin, bsend.at[4], brecv.at[4], (twin, tp))
    part_copy.start()

    each(PART, columns, join)
    each(1, columns, lambda j: returning(0, j).wait_recv())
    each(0, columns, lambda j: returning(2, j).wait_recv())

    def gather(n, carry):
        cols = pl.ds(pl.multiple_of(n * TILE, TILE), TILE)
        acc[:, cols] = combine(wown, 0, cols) + combine(wcross, 2, cols)
        return carry

    lax.fori_loop(0, width // TILE, gather, 0)
    part_copy.wait()
    ffn = acc[...] + pin[...].astype(F32)
    inverse = lax.rsqrt(jnp.mean(ffn * ffn, axis=-1, keepdims=True) + EPS)
    out[...] = (mid[...].astype(F32) + ffn * inverse * post_ffn[...]).astype(BF16)

    raw_copy.wait_send()

    def drain(j):
        for kind in range(3):
            @pl.when((j > 0) | (kind == 2))
            def _():
                outgoing(kind, j).wait_send()
                returning(kind, j).wait_send()
        pass_on(j).wait_send()
        halves(j).wait_send()

    each(0, columns, drain)


def body(
    residual, projected, group_weight, channel_scale, out_weight, post_mix_gain, pre_ffn_gain,
    post_ffn_gain, route_ids, route_weight, expert_gate, expert_up, expert_down,
):
    n_sp = lax.axis_size("sp")
    rows, width = residual.shape
    lines, local_width = projected.shape
    look = 16
    cap = 4 * rows // (n_sp // 2)
    quarter = expert_gate.shape[2]
    hidden = 2 * quarter
    slots = SIDE * SIDE * cap
    any_, vmem = pl.BlockSpec(memory_space=pl.ANY), pl.BlockSpec(memory_space=pltpu.VMEM)
    dma = pltpu.SemaphoreType.DMA
    return pl.pallas_call(
        layer,
        name="layer",
        out_shape=jax.ShapeDtypeStruct((rows, width), BF16),
        in_specs=[any_, any_, any_, vmem, any_, vmem, vmem, vmem, vmem, vmem, any_, any_, any_],
        out_specs=vmem,
        scratch_shapes=[
            pltpu.VMEM((look + lines, local_width), BF16),
            pltpu.VMEM(group_weight.shape, BF16),
            pltpu.VMEM(out_weight.shape, BF16),
            pltpu.VMEM((rows, width), BF16),
            pltpu.VMEM((lines, local_width), BF16),
            pltpu.VMEM((rows, local_width), BF16),
            pltpu.VMEM((rows, width), BF16),
            pltpu.VMEM((rows, width), BF16),
            pltpu.VMEM((rows, width), BF16),
            pltpu.VMEM((3, slots, rows), BF16),
            pltpu.VMEM((3, slots, width), BF16),
            pltpu.VMEM((4, slots, width), BF16),
            pltpu.VMEM((4, slots, width), BF16),
            pltpu.VMEM((slots, width), BF16),
            pltpu.VMEM((3, slots, width), BF16),
            pltpu.VMEM((width, hidden), BF16),
            pltpu.VMEM((width, hidden), BF16),
            pltpu.VMEM((hidden, width), BF16),
            pltpu.VMEM((slots, hidden), BF16),
            pltpu.VMEM((2 * rows, slots), BF16),
            pltpu.VMEM((2 * rows, slots), BF16),
            pltpu.VMEM((2 * rows, slots), BF16),
            pltpu.VMEM((rows, width), F32),
            pltpu.VMEM((rows, width), BF16),
            pltpu.VMEM((rows, width), BF16),
            pltpu.VMEM((2, rows), jnp.int32),
            pltpu.VMEM((2, rows), F32),
            dma((7,)),
            dma((3,)),
            dma((3,)),
            dma((2,)),
            dma((2,)),
            dma((8, SIDE * SIDE)),
            dma((8, SIDE * SIDE)),
            dma((5,)),
            dma((5,)),
        ],
        compiler_params=pltpu.CompilerParams(
            collective_id=0, has_side_effects=True, vmem_limit_bytes=66_000_000
        ),
    )(
        residual, projected, group_weight, channel_scale.reshape(1, -1), out_weight,
        post_mix_gain.reshape(1, -1), pre_ffn_gain.reshape(1, -1), post_ffn_gain.reshape(1, -1),
        route_ids.T, route_weight.T, expert_gate, expert_up, expert_down,
    )


def solution(mesh):
    in_specs = (
        P(("sp", "tp"), None),
        P("sp", "tp"),
        P("tp", None, None),
        P("tp"),
        P(),
        P(),
        P(),
        P(),
        P(("sp", "tp"), None),
        P(("sp", "tp"), None),
        P("sp", None, "tp"),
        P("sp", None, "tp"),
        P("sp", "tp", None),
    )
    out_specs = P(("sp", "tp"), None)
    return jax.shard_map(body, mesh=mesh, in_specs=in_specs, out_specs=out_specs, check_vma=False)
```

```python
import functools

import jax
import jax.numpy as jnp
from jax import lax
from jax.experimental import pallas as pl
from jax.experimental.pallas import tpu as pltpu
from jax.sharding import PartitionSpec as P

EPS = 1e-06
MESH = pl.DeviceIdType.MESH
F32 = jnp.float32
BF16 = jnp.bfloat16
SIDE = 4
PART = 8
EARLY = 8
JOINED = 16
TILE = 256


def dot(a, b):
    return jnp.dot(a, b, preferred_element_type=F32)


def flag(condition):
    return jnp.where(condition, 1.0, 0.0).astype(F32)


def layer(
    res_h, proj_h, gw_h, cs, ow_h, post_mix, pre_ffn, post_ffn, ids_t, wts_t, eg_h, eu_h, ed_h,
    out,
    pbuf, gw, ow, res, scaled, token, mid, normed, raw, pick, table, rbuf, obuf, hbuf, rr, gf, uf, df,
    act, wown, wcross, wpair, acc, pout, pin, ids_t2, wts_t2,
    lsem, wsem, wrem, hsem, tsem, xsend, xrecv, bsend, brecv,
):
    sp = lax.axis_index("sp")
    tp = lax.axis_index("tp")
    other = 1 - tp
    n_sp = lax.axis_size("sp")
    z, y, x = sp // (SIDE * SIDE), (sp // SIDE) % SIDE, sp % SIDE
    rows = out.shape[0]
    width = out.shape[1]
    half_width = width // 2
    cap = 4 * rows // (n_sp // 2)
    quarter = eg_h.shape[2]
    look = pbuf.shape[0] - 2 * rows
    columns = SIDE * SIDE
    slots = columns * cap
    zy = z * SIDE + y
    pair = x // 2
    facing = SIDE - 1 - x
    twin = sp + 1 - 2 * (x % 2)

    def step_of(j):
        dy = j % SIDE
        return (j // SIDE + SIDE - dy) % SIDE, dy

    def ahead(j):
        dz, dy = step_of(j)
        return ((z + dz) % SIDE) * SIDE + (y + dy) % SIDE

    def behind(j):
        dz, dy = step_of(j)
        return ((z + SIDE - dz) % SIDE) * SIDE + (y + SIDE - dy) % SIDE

    def block(j):
        return pl.ds(pl.multiple_of(j * cap, cap), cap)

    def spot(kind, j):
        if kind < 2:
            return kind, block(j)
        first = PART if kind == 3 else SIDE * SIDE - PART
        late = jnp.where(j >= first, 1, 0)
        place = j - late * first + (kind - 2) * jnp.where(late == 1, PART, SIDE * SIDE - PART)
        return 2 + late, block(place)

    def each(low, high, act_on):
        def step(k, carry):
            act_on(k)
            return carry

        lax.fori_loop(low, high, step, 0)

    def remote(src, dst, send, recv, device):
        return pltpu.make_async_remote_copy(
            src_ref=src, dst_ref=dst, send_sem=send, recv_sem=recv, device_id=device, device_id_type=MESH
        )

    barrier = pltpu.get_barrier_semaphore()

    def greet(device):
        pl.semaphore_signal(barrier, inc=1, device_id=device, device_id_type=MESH)

    each(1, columns, lambda j: greet((ahead(j) * SIDE + x, tp)))
    each(0, columns, lambda j: greet((ahead(j) * SIDE + facing, tp)))
    greet((twin, tp))
    greet((sp, other))

    own_cols = pl.ds(pl.multiple_of(tp * quarter, 128), quarter)
    own_rows = pl.ds(pl.multiple_of(tp * quarter, 128), quarter)
    local = [
        pltpu.make_async_copy(proj_h, pbuf.at[pl.ds(look, 2 * rows)], lsem.at[0]),
        pltpu.make_async_copy(gw_h, gw, lsem.at[1]),
        pltpu.make_async_copy(ow_h, ow, lsem.at[2]),
        pltpu.make_async_copy(res_h, res, lsem.at[3]),
        pltpu.make_async_copy(eg_h.at[0], gf.at[:, own_cols], lsem.at[4]),
        pltpu.make_async_copy(eu_h.at[0], uf.at[:, own_cols], lsem.at[5]),
        pltpu.make_async_copy(ed_h.at[0], df.at[own_rows], lsem.at[6]),
    ]
    for copy in local:
        copy.start()

    experts = n_sp // 2
    r0 = lax.broadcasted_iota(jnp.int32, (rows, rows), 0)
    r1 = lax.broadcasted_iota(jnp.int32, (rows, rows), 1)
    e_sub = lax.broadcasted_iota(jnp.int32, (experts, rows), 0)
    e_lane = lax.broadcasted_iota(jnp.int32, (rows, experts), 1)
    s0 = lax.broadcasted_iota(jnp.int32, (slots, experts), 0)
    s1 = lax.broadcasted_iota(jnp.int32, (slots, experts), 1)
    q0 = lax.broadcasted_iota(jnp.int32, (experts, slots), 0)
    q1 = lax.broadcasted_iota(jnp.int32, (experts, slots), 1)
    place = (lax.broadcasted_iota(jnp.int32, (slots, rows), 0) % cap).astype(F32)
    lane_place = (lax.broadcasted_iota(jnp.int32, (rows, slots), 1) % cap).astype(F32)

    def named_slots(names):
        named = flag(e_sub == names[0:1, :]) + flag(e_sub == names[1:2, :])
        return named.astype(BF16), dot(named.astype(BF16), flag(r0 < r1).astype(BF16)).astype(BF16)

    def picks(slot_info, side):
        spread = flag((s0 // cap) * 2 + side == s1).astype(BF16)
        hit = dot(spread, slot_info[0]) > 0.5
        return flag(hit & (dot(spread, slot_info[1]) == place)).astype(BF16)

    def row_info(names, values):
        sheet = [names[0:2, :].astype(F32), values[0:2, :], jnp.zeros((4, rows), F32)]
        sheet = jnp.transpose(jnp.concatenate(sheet, axis=0))
        lane = e_lane.astype(F32)
        first, second = flag(lane == sheet[:, 0:1]), flag(lane == sheet[:, 1:2])
        named = (first + second).astype(BF16)
        before = dot(flag(r1 < r0).astype(BF16), named).astype(BF16)
        weight = first * sheet[:, 2:3] + second * sheet[:, 3:4]
        high = weight.astype(BF16)
        return named, before, high, (weight - high.astype(F32)).astype(BF16)

    def weigh(ref, info, side):
        named, before, high, low = info
        spread = flag((q1 // cap) * 2 + side == q0).astype(BF16)
        here = (dot(named, spread) > 0.5) & (dot(before, spread) == lane_place)
        ref[0:rows] = jnp.where(here, dot(high, spread), 0.0).astype(BF16)
        ref[rows : 2 * rows] = jnp.where(here, dot(low, spread), 0.0).astype(BF16)

    own_slots = named_slots(ids_t)
    pick[0] = picks(own_slots, pair)
    pick[1] = picks(own_slots, 1 - pair)
    own_info = row_info(ids_t, wts_t)
    weigh(wown, own_info, pair)
    weigh(wcross, own_info, 1 - pair)

    local[0].wait()
    pl.semaphore_wait(barrier, 2 * columns + 1)
    notes = [
        remote(src, dst, bsend.at[i], brecv.at[i], (twin, tp))
        for i, (src, dst) in enumerate(((ids_t, ids_t2), (wts_t, wts_t2)))
    ]

    halo = remote(
        pbuf.at[pl.ds(2 * rows, look)], pbuf.at[pl.ds(0, look)], hsem.at[0], hsem.at[1],
        ((sp + 1) % n_sp, tp),
    )
    halo.start()
    for note in notes:
        note.start()
    pushes = [
        remote(src, dst, wsem.at[i], wrem.at[i], (sp, other))
        for i, (src, dst) in enumerate(
            (
                (eg_h.at[0], gf.at[:, own_cols]),
                (eu_h.at[0], uf.at[:, own_cols]),
                (ed_h.at[0], df.at[own_rows]),
            )
        )
    ]

    local[1].wait()
    group = gw.shape[1]

    def pool(extended, lg, start, known):
        count = extended.shape[0]
        row_id = lax.broadcasted_iota(jnp.int32, (count, group), 0)
        own = extended.astype(F32)
        if known is not None:
            own = jnp.where((row_id >= look) | known, own, 0.0)
        sums = [own]
        for level in range(4):
            sums.append(pltpu.roll(sums[-1], 2**level, 0) + sums[-1])
        summed = jnp.where(tp == 0, sums[lg + 1], sums[lg + 3])
        span = jnp.where(tp == 0, F32(2.0 ** (lg + 1)), F32(2.0 ** (lg + 3)))
        position = (row_id - look + 1 + start + sp * (2 * rows)).astype(F32)
        return (summed / jnp.minimum(position, span) - own).astype(BF16)[look:]

    def columns_of(lg):
        return slice(lg * group, (lg + 1) * group)

    for lg in range(2):
        cols = columns_of(lg)
        pooled = pool(pbuf[look:, cols], lg, look, None)
        scaled[look:, cols] = (dot(pooled, gw[lg]) * cs[:, cols]).astype(BF16)
    halo.wait()
    for lg in range(2):
        cols = columns_of(lg)
        pooled = pool(pbuf[0 : 2 * look, cols], lg, 0, sp > 0)
        scaled[0:look, cols] = (dot(pooled, gw[lg]) * cs[:, cols]).astype(BF16)

    swap = remote(
        scaled.at[pl.ds(pl.multiple_of(other * rows, rows), rows)], token, tsem.at[0], tsem.at[1],
        (sp, other),
    )
    swap.start()
    local[2].wait()
    local[3].wait()
    mine = pl.ds(pl.multiple_of(tp * rows, rows), rows)

    def project(source, part, accumulate):
        def step(n, carry):
            cols = pl.ds(pl.multiple_of(n * TILE, TILE), TILE)
            part_rows = ow[pl.ds(pl.multiple_of(part * half_width, half_width), half_width), cols]
            value = dot(source, part_rows)
            acc[:, cols] = acc[:, cols] + value if accumulate else value
            return carry

        lax.fori_loop(0, width // TILE, step, 0)

    project(scaled[mine], tp, False)
    swap.wait()
    for push in pushes:
        push.start()
    project(token[...], other, True)

    mixed = acc[...].astype(BF16).astype(F32)
    inverse = lax.rsqrt(jnp.mean(mixed * mixed, axis=-1, keepdims=True) + EPS)
    middle = (res[...].astype(F32) + mixed * inverse * post_mix[...]).astype(BF16)
    mid[...] = middle
    middle = middle.astype(F32)
    inverse = lax.rsqrt(jnp.mean(middle * middle, axis=-1, keepdims=True) + EPS)
    normed[...] = (middle * inverse * pre_ffn[...]).astype(BF16)

    raw_copy = remote(normed, raw, bsend.at[3], brecv.at[3], (twin, tp))
    raw_copy.start()

    def fill(kind, source):
        def step(n, carry):
            cols = pl.ds(pl.multiple_of(n * TILE, TILE), TILE)
            table[kind, :, cols] = dot(pick[kind], source[:, cols]).astype(BF16)
            return carry

        lax.fori_loop(0, width // TILE, step, 0)

    def outgoing(kind, j):
        peer = ahead(j)
        line = facing if kind == 2 else x
        return remote(
            table.at[(0, 2, 1)[kind], block(peer)], rbuf.at[spot(kind, j)],
            xsend.at[kind, j], xrecv.at[kind, j], (peer * SIDE + line, tp),
        )

    def pass_on(j):
        return remote(rbuf.at[spot(2, j)], rbuf.at[spot(3, j)], xsend.at[3, j], xrecv.at[3, j], (twin, tp))

    def returning(kind, j):
        line = facing if kind == 2 else x
        return remote(
            obuf.at[spot(kind, j)], rr.at[kind, block(zy)],
            xsend.at[4 + kind, j], xrecv.at[4 + kind, j], (behind(j) * SIDE + line, tp),
        )

    def halves(j):
        return remote(obuf.at[spot(3, j)], hbuf.at[block(j)], xsend.at[7, j], xrecv.at[7, j], (twin, tp))

    fill(1, normed)
    each(0, columns, lambda j: outgoing(2, j).start())
    fill(0, normed)
    each(1, columns, lambda j: outgoing(0, j).start())
    rbuf[0, 0:cap] = table[0, block(zy)]

    def relay(j):
        outgoing(2, j).wait_recv()
        pass_on(j).start()

    for note in notes:
        note.wait()
    pick[2] = picks(named_slots(ids_t2), pair)
    weigh(wpair, row_info(ids_t2, wts_t2), pair)
    each(0, EARLY, relay)
    raw_copy.wait_recv()
    fill(2, raw)
    each(1, columns, lambda j: outgoing(1, j).start())
    rbuf[1, 0:cap] = table[2, block(zy)]

    for copy in local[4:]:
        copy.wait()
    for push in pushes:
        push.wait()

    hidden = gf.shape[1]

    def join(j):
        halves(j).wait_recv()
        both = obuf[spot(2, j)].astype(F32) + hbuf[block(j)].astype(F32)
        obuf[spot(2, j)] = both.astype(BF16)
        returning(2, j).start()

    some = (columns - EARLY) // 4

    def expert_unit(u, carry):
        c = (u % 2) * 2 + u // 2

        @pl.when(u == 0)
        def _():
            each(1, columns, lambda j: outgoing(0, j).wait_recv())

        @pl.when(u == 1)
        def _():
            each(0, PART, lambda j: pass_on(j).wait_recv())

        @pl.when(u == 2)
        def _():
            each(1, columns, lambda j: outgoing(1, j).wait_recv())

        @pl.when(u == 3)
        def _():
            each(PART, columns, lambda j: pass_on(j).wait_recv())

        def relays(low, high):
            @pl.when(u == 0)
            def _():
                each(low, high, relay)

        gate = dot(rbuf[c], gf[...])
        relays(EARLY, EARLY + some)
        act[...] = (jax.nn.silu(gate) * dot(rbuf[c], uf[...])).astype(BF16)
        relays(EARLY + some, EARLY + 2 * some)
        obuf[c] = dot(act[...], df[...]).astype(BF16)
        relays(EARLY + 2 * some, columns)

        @pl.when(u == 0)
        def _():
            each(1, columns, lambda j: returning(0, j).start())
            rr[0, block(zy)] = obuf[0, 0:cap]

        @pl.when(u == 1)
        def _():
            each(0, PART, lambda j: halves(j).start())

        @pl.when(u == 2)
        def _():
            each(1, columns, lambda j: returning(1, j).start())
            rr[1, block(zy)] = obuf[1, 0:cap]

        @pl.when(u == 3)
        def _():
            each(PART, columns, lambda j: halves(j).start())

        return carry

    lax.fori_loop(0, 4, expert_unit, 0)

    def combine(weights, kind, cols):
        both = dot(weights[...], rr[kind, :, cols])
        return both[0:rows] + both[rows : 2 * rows]

    each(0, JOINED, join)
    each(1, columns, lambda j: returning(1, j).wait_recv())

    def give(n, carry):
        cols = pl.ds(pl.multiple_of(n * TILE, TILE), TILE)
        pout[:, cols] = combine(wpair, 1, cols).astype(BF16)
        return carry

    lax.fori_loop(0, width // TILE, give, 0)
    part_copy = remote(pout, pin, bsend.at[4], brecv.at[4], (twin, tp))
    part_copy.start()
    each(JOINED, columns, join)

    each(1, columns, lambda j: returning(0, j).wait_recv())
    each(0, columns, lambda j: returning(2, j).wait_recv())

    def gather(n, carry):
        cols = pl.ds(pl.multiple_of(n * TILE, TILE), TILE)
        acc[:, cols] = combine(wown, 0, cols) + combine(wcross, 2, cols)
        return carry

    lax.fori_loop(0, width // TILE, gather, 0)
    part_copy.wait()
    ffn = acc[...] + pin[...].astype(F32)
    inverse = lax.rsqrt(jnp.mean(ffn * ffn, axis=-1, keepdims=True) + EPS)
    out[...] = (mid[...].astype(F32) + ffn * inverse * post_ffn[...]).astype(BF16)

    raw_copy.wait_send()

    def drain(j):
        for kind in range(3):
            @pl.when((j > 0) | (kind == 2))
            def _():
                outgoing(kind, j).wait_send()
                returning(kind, j).wait_send()
        pass_on(j).wait_send()
        halves(j).wait_send()

    each(0, columns, drain)


def body(
    residual, projected, group_weight, channel_scale, out_weight, post_mix_gain, pre_ffn_gain,
    post_ffn_gain, route_ids, route_weight, expert_gate, expert_up, expert_down,
):
    n_sp = lax.axis_size("sp")
    rows, width = residual.shape
    lines, local_width = projected.shape
    look = 16
    cap = 4 * rows // (n_sp // 2)
    quarter = expert_gate.shape[2]
    hidden = 2 * quarter
    slots = SIDE * SIDE * cap
    any_, vmem = pl.BlockSpec(memory_space=pl.ANY), pl.BlockSpec(memory_space=pltpu.VMEM)
    dma = pltpu.SemaphoreType.DMA
    return pl.pallas_call(
        layer,
        name="layer",
        out_shape=jax.ShapeDtypeStruct((rows, width), BF16),
        in_specs=[any_, any_, any_, vmem, any_, vmem, vmem, vmem, vmem, vmem, any_, any_, any_],
        out_specs=vmem,
        scratch_shapes=[
            pltpu.VMEM((look + lines, local_width), BF16),
            pltpu.VMEM(group_weight.shape, BF16),
            pltpu.VMEM(out_weight.shape, BF16),
            pltpu.VMEM((rows, width), BF16),
            pltpu.VMEM((lines, local_width), BF16),
            pltpu.VMEM((rows, local_width), BF16),
            pltpu.VMEM((rows, width), BF16),
            pltpu.VMEM((rows, width), BF16),
            pltpu.VMEM((rows, width), BF16),
            pltpu.VMEM((3, slots, rows), BF16),
            pltpu.VMEM((3, slots, width), BF16),
            pltpu.VMEM((4, slots, width), BF16),
            pltpu.VMEM((4, slots, width), BF16),
            pltpu.VMEM((slots, width), BF16),
            pltpu.VMEM((3, slots, width), BF16),
            pltpu.VMEM((width, hidden), BF16),
            pltpu.VMEM((width, hidden), BF16),
            pltpu.VMEM((hidden, width), BF16),
            pltpu.VMEM((slots, hidden), BF16),
            pltpu.VMEM((2 * rows, slots), BF16),
            pltpu.VMEM((2 * rows, slots), BF16),
            pltpu.VMEM((2 * rows, slots), BF16),
            pltpu.VMEM((rows, width), F32),
            pltpu.VMEM((rows, width), BF16),
            pltpu.VMEM((rows, width), BF16),
            pltpu.VMEM((2, rows), jnp.int32),
            pltpu.VMEM((2, rows), F32),
            dma((7,)),
            dma((3,)),
            dma((3,)),
            dma((2,)),
            dma((2,)),
            dma((8, SIDE * SIDE)),
            dma((8, SIDE * SIDE)),
            dma((5,)),
            dma((5,)),
        ],
        compiler_params=pltpu.CompilerParams(
            collective_id=0, has_side_effects=True, vmem_limit_bytes=66_000_000
        ),
    )(
        residual, projected, group_weight, channel_scale.reshape(1, -1), out_weight,
        post_mix_gain.reshape(1, -1), pre_ffn_gain.reshape(1, -1), post_ffn_gain.reshape(1, -1),
        route_ids.T, route_weight.T, expert_gate, expert_up, expert_down,
    )


def solution(mesh):
    in_specs = (
        P(("sp", "tp"), None),
        P("sp", "tp"),
        P("tp", None, None),
        P("tp"),
        P(),
        P(),
        P(),
        P(),
        P(("sp", "tp"), None),
        P(("sp", "tp"), None),
        P("sp", None, "tp"),
        P("sp", None, "tp"),
        P("sp", "tp", None),
    )
    out_specs = P(("sp", "tp"), None)
    return jax.shard_map(body, mesh=mesh, in_specs=in_specs, out_specs=out_specs, check_vma=False)
```

```python
import functools

import jax
import jax.numpy as jnp
from jax import lax
from jax.experimental import pallas as pl
from jax.experimental.pallas import tpu as pltpu
from jax.sharding import PartitionSpec as P

EPS = 1e-06
MESH = pl.DeviceIdType.MESH
F32 = jnp.float32
BF16 = jnp.bfloat16
SIDE = 4
PART = 8
EARLY = 8
JOINED = 16
TILE = 256


def dot(a, b):
    return jnp.dot(a, b, preferred_element_type=F32)


def flag(condition):
    return jnp.where(condition, 1.0, 0.0).astype(F32)


def layer(
    res_h, proj_h, gw_h, cs, ow_h, post_mix, pre_ffn, post_ffn, ids_t, wts_t, eg_h, eu_h, ed_h,
    out,
    pbuf, gw, ow, res, scaled, token, mid, normed, raw, pick, table, rbuf, obuf, hbuf, rr, gf, uf, df,
    act, wown, wcross, wpair, acc, pout, pin, ids_t2, wts_t2,
    lsem, wsem, wrem, hsem, tsem, xsend, xrecv, bsend, brecv,
):
    sp = lax.axis_index("sp")
    tp = lax.axis_index("tp")
    other = 1 - tp
    n_sp = lax.axis_size("sp")
    z, y, x = sp // (SIDE * SIDE), (sp // SIDE) % SIDE, sp % SIDE
    rows = out.shape[0]
    width = out.shape[1]
    half_width = width // 2
    cap = 4 * rows // (n_sp // 2)
    quarter = eg_h.shape[2]
    look = pbuf.shape[0] - 2 * rows
    columns = SIDE * SIDE
    slots = columns * cap
    zy = z * SIDE + y
    pair = x // 2
    facing = SIDE - 1 - x
    twin = sp + 1 - 2 * (x % 2)

    def step_of(j):
        dy = j % SIDE
        return (j // SIDE + SIDE - dy) % SIDE, dy

    def ahead(j):
        dz, dy = step_of(j)
        return ((z + dz) % SIDE) * SIDE + (y + dy) % SIDE

    def behind(j):
        dz, dy = step_of(j)
        return ((z + SIDE - dz) % SIDE) * SIDE + (y + SIDE - dy) % SIDE

    def block(j):
        return pl.ds(pl.multiple_of(j * cap, cap), cap)

    def spot(kind, j):
        if kind < 2:
            return kind, block(j)
        first = PART if kind == 3 else SIDE * SIDE - PART
        late = jnp.where(j >= first, 1, 0)
        place = j - late * first + (kind - 2) * jnp.where(late == 1, PART, SIDE * SIDE - PART)
        return 2 + late, block(place)

    def each(low, high, act_on):
        def step(k, carry):
            act_on(k)
            return carry

        lax.fori_loop(low, high, step, 0)

    def remote(src, dst, send, recv, device):
        return pltpu.make_async_remote_copy(
            src_ref=src, dst_ref=dst, send_sem=send, recv_sem=recv, device_id=device, device_id_type=MESH
        )

    barrier = pltpu.get_barrier_semaphore()

    def greet(device):
        pl.semaphore_signal(barrier, inc=1, device_id=device, device_id_type=MESH)

    each(1, columns, lambda j: greet((ahead(j) * SIDE + x, tp)))
    each(0, columns, lambda j: greet((ahead(j) * SIDE + facing, tp)))
    greet((twin, tp))
    greet((sp, other))

    own_cols = pl.ds(pl.multiple_of(tp * quarter, 128), quarter)
    own_rows = pl.ds(pl.multiple_of(tp * quarter, 128), quarter)
    local = [
        pltpu.make_async_copy(proj_h, pbuf.at[pl.ds(look, 2 * rows)], lsem.at[0]),
        pltpu.make_async_copy(gw_h, gw, lsem.at[1]),
        pltpu.make_async_copy(ow_h, ow, lsem.at[2]),
        pltpu.make_async_copy(res_h, res, lsem.at[3]),
        pltpu.make_async_copy(eg_h.at[0], gf.at[:, own_cols], lsem.at[4]),
        pltpu.make_async_copy(eu_h.at[0], uf.at[:, own_cols], lsem.at[5]),
        pltpu.make_async_copy(ed_h.at[0], df.at[own_rows], lsem.at[6]),
    ]
    for copy in local[:4]:
        copy.start()

    experts = n_sp // 2
    r0 = lax.broadcasted_iota(jnp.int32, (rows, rows), 0)
    r1 = lax.broadcasted_iota(jnp.int32, (rows, rows), 1)
    e_sub = lax.broadcasted_iota(jnp.int32, (experts, rows), 0)
    e_lane = lax.broadcasted_iota(jnp.int32, (rows, experts), 1)
    s0 = lax.broadcasted_iota(jnp.int32, (slots, experts), 0)
    s1 = lax.broadcasted_iota(jnp.int32, (slots, experts), 1)
    q0 = lax.broadcasted_iota(jnp.int32, (experts, slots), 0)
    q1 = lax.broadcasted_iota(jnp.int32, (experts, slots), 1)
    place = (lax.broadcasted_iota(jnp.int32, (slots, rows), 0) % cap).astype(F32)
    lane_place = (lax.broadcasted_iota(jnp.int32, (rows, slots), 1) % cap).astype(F32)

    def named_slots(names):
        named = flag(e_sub == names[0:1, :]) + flag(e_sub == names[1:2, :])
        return named.astype(BF16), dot(named.astype(BF16), flag(r0 < r1).astype(BF16)).astype(BF16)

    def picks(slot_info, side):
        spread = flag((s0 // cap) * 2 + side == s1).astype(BF16)
        hit = dot(spread, slot_info[0]) > 0.5
        return flag(hit & (dot(spread, slot_info[1]) == place)).astype(BF16)

    def row_info(names, values):
        sheet = [names[0:2, :].astype(F32), values[0:2, :], jnp.zeros((4, rows), F32)]
        sheet = jnp.transpose(jnp.concatenate(sheet, axis=0))
        lane = e_lane.astype(F32)
        first, second = flag(lane == sheet[:, 0:1]), flag(lane == sheet[:, 1:2])
        named = (first + second).astype(BF16)
        before = dot(flag(r1 < r0).astype(BF16), named).astype(BF16)
        weight = first * sheet[:, 2:3] + second * sheet[:, 3:4]
        high = weight.astype(BF16)
        return named, before, high, (weight - high.astype(F32)).astype(BF16)

    def weigh(ref, info, side):
        named, before, high, low = info
        spread = flag((q1 // cap) * 2 + side == q0).astype(BF16)
        here = (dot(named, spread) > 0.5) & (dot(before, spread) == lane_place)
        ref[0:rows] = jnp.where(here, dot(high, spread), 0.0).astype(BF16)
        ref[rows : 2 * rows] = jnp.where(here, dot(low, spread), 0.0).astype(BF16)

    own_slots = named_slots(ids_t)
    pick[0] = picks(own_slots, pair)
    pick[1] = picks(own_slots, 1 - pair)
    own_info = row_info(ids_t, wts_t)
    weigh(wown, own_info, pair)
    weigh(wcross, own_info, 1 - pair)

    local[0].wait()
    pl.semaphore_wait(barrier, 2 * columns + 1)
    notes = [
        remote(src, dst, bsend.at[i], brecv.at[i], (twin, tp))
        for i, (src, dst) in enumerate(((ids_t, ids_t2), (wts_t, wts_t2)))
    ]

    halo = remote(
        pbuf.at[pl.ds(2 * rows, look)], pbuf.at[pl.ds(0, look)], hsem.at[0], hsem.at[1],
        ((sp + 1) % n_sp, tp),
    )
    halo.start()
    for note in notes:
        note.start()
    pushes = [
        remote(src, dst, wsem.at[i], wrem.at[i], (sp, other))
        for i, (src, dst) in enumerate(
            (
                (eg_h.at[0], gf.at[:, own_cols]),
                (eu_h.at[0], uf.at[:, own_cols]),
                (ed_h.at[0], df.at[own_rows]),
            )
        )
    ]

    local[1].wait()
    group = gw.shape[1]

    def pool(extended, lg, start, known):
        count = extended.shape[0]
        row_id = lax.broadcasted_iota(jnp.int32, (count, group), 0)
        own = extended.astype(F32)
        if known is not None:
            own = jnp.where((row_id >= look) | known, own, 0.0)
        sums = [own]
        for level in range(4):
            sums.append(pltpu.roll(sums[-1], 2**level, 0) + sums[-1])
        summed = jnp.where(tp == 0, sums[lg + 1], sums[lg + 3])
        span = jnp.where(tp == 0, F32(2.0 ** (lg + 1)), F32(2.0 ** (lg + 3)))
        position = (row_id - look + 1 + start + sp * (2 * rows)).astype(F32)
        return (summed / jnp.minimum(position, span) - own).astype(BF16)[look:]

    def columns_of(lg):
        return slice(lg * group, (lg + 1) * group)

    for lg in range(2):
        cols = columns_of(lg)
        pooled = pool(pbuf[look:, cols], lg, look, None)
        scaled[look:, cols] = (dot(pooled, gw[lg]) * cs[:, cols]).astype(BF16)
    halo.wait()
    for lg in range(2):
        cols = columns_of(lg)
        pooled = pool(pbuf[0 : 2 * look, cols], lg, 0, sp > 0)
        scaled[0:look, cols] = (dot(pooled, gw[lg]) * cs[:, cols]).astype(BF16)

    swap = remote(
        scaled.at[pl.ds(pl.multiple_of(other * rows, rows), rows)], token, tsem.at[0], tsem.at[1],
        (sp, other),
    )
    swap.start()
    for copy in local[4:]:
        copy.start()
    local[2].wait()
    local[3].wait()
    mine = pl.ds(pl.multiple_of(tp * rows, rows), rows)

    def project(source, part, accumulate):
        def step(n, carry):
            cols = pl.ds(pl.multiple_of(n * TILE, TILE), TILE)
            part_rows = ow[pl.ds(pl.multiple_of(part * half_width, half_width), half_width), cols]
            value = dot(source, part_rows)
            acc[:, cols] = acc[:, cols] + value if accumulate else value
            return carry

        lax.fori_loop(0, width // TILE, step, 0)

    project(scaled[mine], tp, False)
    swap.wait()
    project(token[...], other, True)

    mixed = acc[...].astype(BF16).astype(F32)
    inverse = lax.rsqrt(jnp.mean(mixed * mixed, axis=-1, keepdims=True) + EPS)
    middle = (res[...].astype(F32) + mixed * inverse * post_mix[...]).astype(BF16)
    mid[...] = middle
    middle = middle.astype(F32)
    inverse = lax.rsqrt(jnp.mean(middle * middle, axis=-1, keepdims=True) + EPS)
    normed[...] = (middle * inverse * pre_ffn[...]).astype(BF16)

    raw_copy = remote(normed, raw, bsend.at[3], brecv.at[3], (twin, tp))
    raw_copy.start()

    def fill(kind, source):
        def step(n, carry):
            cols = pl.ds(pl.multiple_of(n * TILE, TILE), TILE)
            table[kind, :, cols] = dot(pick[kind], source[:, cols]).astype(BF16)
            return carry

        lax.fori_loop(0, width // TILE, step, 0)

    def outgoing(kind, j):
        peer = ahead(j)
        line = facing if kind == 2 else x
        return remote(
            table.at[(0, 2, 1)[kind], block(peer)], rbuf.at[spot(kind, j)],
            xsend.at[kind, j], xrecv.at[kind, j], (peer * SIDE + line, tp),
        )

    def pass_on(j):
        return remote(rbuf.at[spot(2, j)], rbuf.at[spot(3, j)], xsend.at[3, j], xrecv.at[3, j], (twin, tp))

    def returning(kind, j):
        line = facing if kind == 2 else x
        return remote(
            obuf.at[spot(kind, j)], rr.at[kind, block(zy)],
            xsend.at[4 + kind, j], xrecv.at[4 + kind, j], (behind(j) * SIDE + line, tp),
        )

    def halves(j):
        return remote(obuf.at[spot(3, j)], hbuf.at[block(j)], xsend.at[7, j], xrecv.at[7, j], (twin, tp))

    fill(1, normed)
    each(0, columns, lambda j: outgoing(2, j).start())
    fill(0, normed)
    each(1, columns, lambda j: outgoing(0, columns - j).start())
    for push in pushes:
        push.start()
    rbuf[0, 0:cap] = table[0, block(zy)]

    def relay(j):
        outgoing(2, j).wait_recv()
        pass_on(j).start()

    for note in notes:
        note.wait()
    pick[2] = picks(named_slots(ids_t2), pair)
    weigh(wpair, row_info(ids_t2, wts_t2), pair)
    each(0, EARLY, relay)
    raw_copy.wait_recv()
    fill(2, raw)
    each(1, columns, lambda j: outgoing(1, j).start())
    rbuf[1, 0:cap] = table[2, block(zy)]

    for copy in local[4:]:
        copy.wait()
    for push in pushes:
        push.wait()

    hidden = gf.shape[1]

    def join(j):
        halves(j).wait_recv()
        both = obuf[spot(2, j)].astype(F32) + hbuf[block(j)].astype(F32)
        obuf[spot(2, j)] = both.astype(BF16)
        returning(2, j).start()

    some = (columns - EARLY) // 4

    def expert_unit(u, carry):
        c = (u % 2) * 2 + u // 2

        @pl.when(u == 0)
        def _():
            each(1, columns, lambda j: outgoing(0, j).wait_recv())

        @pl.when(u == 1)
        def _():
            each(0, PART, lambda j: pass_on(j).wait_recv())

        @pl.when(u == 2)
        def _():
            each(1, columns, lambda j: outgoing(1, j).wait_recv())

        @pl.when(u == 3)
        def _():
            each(PART, columns, lambda j: pass_on(j).wait_recv())

        def relays(low, high):
            @pl.when(u == 0)
            def _():
                each(low, high, relay)

        gate = dot(rbuf[c], gf[...])
        relays(EARLY, EARLY + some)
        act[...] = (jax.nn.silu(gate) * dot(rbuf[c], uf[...])).astype(BF16)
        relays(EARLY + some, EARLY + 2 * some)
        obuf[c] = dot(act[...], df[...]).astype(BF16)
        relays(EARLY + 2 * some, columns)

        @pl.when(u == 0)
        def _():
            each(1, columns, lambda j: returning(0, j).start())
            rr[0, block(zy)] = obuf[0, 0:cap]

        @pl.when(u == 1)
        def _():
            each(0, PART, lambda j: halves(j).start())

        @pl.when(u == 2)
        def _():
            each(1, columns, lambda j: returning(1, j).start())
            rr[1, block(zy)] = obuf[1, 0:cap]

        @pl.when(u == 3)
        def _():
            each(PART, columns, lambda j: halves(j).start())

        return carry

    lax.fori_loop(0, 4, expert_unit, 0)

    def combine(weights, kind, cols):
        both = dot(weights[...], rr[kind, :, cols])
        return both[0:rows] + both[rows : 2 * rows]

    each(0, JOINED, join)
    each(1, columns, lambda j: returning(1, j).wait_recv())

    def give(n, carry):
        cols = pl.ds(pl.multiple_of(n * TILE, TILE), TILE)
        pout[:, cols] = combine(wpair, 1, cols).astype(BF16)
        return carry

    lax.fori_loop(0, width // TILE, give, 0)
    part_copy = remote(pout, pin, bsend.at[4], brecv.at[4], (twin, tp))
    part_copy.start()
    each(JOINED, columns, join)

    each(1, columns, lambda j: returning(0, j).wait_recv())
    each(0, columns, lambda j: returning(2, j).wait_recv())

    def gather(n, carry):
        cols = pl.ds(pl.multiple_of(n * TILE, TILE), TILE)
        acc[:, cols] = combine(wown, 0, cols) + combine(wcross, 2, cols)
        return carry

    lax.fori_loop(0, width // TILE, gather, 0)
    part_copy.wait()
    ffn = acc[...] + pin[...].astype(F32)
    inverse = lax.rsqrt(jnp.mean(ffn * ffn, axis=-1, keepdims=True) + EPS)
    out[...] = (mid[...].astype(F32) + ffn * inverse * post_ffn[...]).astype(BF16)

    raw_copy.wait_send()

    def drain(j):
        for kind in range(3):
            @pl.when((j > 0) | (kind == 2))
            def _():
                outgoing(kind, j).wait_send()
                returning(kind, j).wait_send()
        pass_on(j).wait_send()
        halves(j).wait_send()

    each(0, columns, drain)


def body(
    residual, projected, group_weight, channel_scale, out_weight, post_mix_gain, pre_ffn_gain,
    post_ffn_gain, route_ids, route_weight, expert_gate, expert_up, expert_down,
):
    n_sp = lax.axis_size("sp")
    rows, width = residual.shape
    lines, local_width = projected.shape
    look = 16
    cap = 4 * rows // (n_sp // 2)
    quarter = expert_gate.shape[2]
    hidden = 2 * quarter
    slots = SIDE * SIDE * cap
    any_, vmem = pl.BlockSpec(memory_space=pl.ANY), pl.BlockSpec(memory_space=pltpu.VMEM)
    dma = pltpu.SemaphoreType.DMA
    return pl.pallas_call(
        layer,
        name="layer",
        out_shape=jax.ShapeDtypeStruct((rows, width), BF16),
        in_specs=[any_, any_, any_, vmem, any_, vmem, vmem, vmem, vmem, vmem, any_, any_, any_],
        out_specs=vmem,
        scratch_shapes=[
            pltpu.VMEM((look + lines, local_width), BF16),
            pltpu.VMEM(group_weight.shape, BF16),
            pltpu.VMEM(out_weight.shape, BF16),
            pltpu.VMEM((rows, width), BF16),
            pltpu.VMEM((lines, local_width), BF16),
            pltpu.VMEM((rows, local_width), BF16),
            pltpu.VMEM((rows, width), BF16),
            pltpu.VMEM((rows, width), BF16),
            pltpu.VMEM((rows, width), BF16),
            pltpu.VMEM((3, slots, rows), BF16),
            pltpu.VMEM((3, slots, width), BF16),
            pltpu.VMEM((4, slots, width), BF16),
            pltpu.VMEM((4, slots, width), BF16),
            pltpu.VMEM((slots, width), BF16),
            pltpu.VMEM((3, slots, width), BF16),
            pltpu.VMEM((width, hidden), BF16),
            pltpu.VMEM((width, hidden), BF16),
            pltpu.VMEM((hidden, width), BF16),
            pltpu.VMEM((slots, hidden), BF16),
            pltpu.VMEM((2 * rows, slots), BF16),
            pltpu.VMEM((2 * rows, slots), BF16),
            pltpu.VMEM((2 * rows, slots), BF16),
            pltpu.VMEM((rows, width), F32),
            pltpu.VMEM((rows, width), BF16),
            pltpu.VMEM((rows, width), BF16),
            pltpu.VMEM((2, rows), jnp.int32),
            pltpu.VMEM((2, rows), F32),
            dma((7,)),
            dma((3,)),
            dma((3,)),
            dma((2,)),
            dma((2,)),
            dma((8, SIDE * SIDE)),
            dma((8, SIDE * SIDE)),
            dma((5,)),
            dma((5,)),
        ],
        compiler_params=pltpu.CompilerParams(
            collective_id=0, has_side_effects=True, vmem_limit_bytes=66_000_000
        ),
    )(
        residual, projected, group_weight, channel_scale.reshape(1, -1), out_weight,
        post_mix_gain.reshape(1, -1), pre_ffn_gain.reshape(1, -1), post_ffn_gain.reshape(1, -1),
        route_ids.T, route_weight.T, expert_gate, expert_up, expert_down,
    )


def solution(mesh):
    in_specs = (
        P(("sp", "tp"), None),
        P("sp", "tp"),
        P("tp", None, None),
        P("tp"),
        P(),
        P(),
        P(),
        P(),
        P(("sp", "tp"), None),
        P(("sp", "tp"), None),
        P("sp", None, "tp"),
        P("sp", None, "tp"),
        P("sp", "tp", None),
    )
    out_specs = P(("sp", "tp"), None)
    return jax.shard_map(body, mesh=mesh, in_specs=in_specs, out_specs=out_specs, check_vma=False)
```
